32 devices in a mesh: ep: 8 (over z, y), tp: 4 (over x, core).
Axes of the slice: x: 2, y: 2, z: 4, core: 2. Of those that a mesh axis runs over, the one named last changes fastest.
Arguments:
- att_queries: bfloat16 [8192, 1024], P(('ep', 'tp')), may hold values from -8 to 8
- att_keys: bfloat16 [8192, 256], P(('ep', 'tp')), may hold values from -6 to 6
- att_values: bfloat16 [8192, 256], P(('ep', 'tp')), may hold values from -6 to 6
- sink_logits: float32 [16], replicated, may hold values from 3 to 6.5
- out_weight: bfloat16 [1024, 2048], replicated, may hold values from -0.1875 to 0.1875
- att_gain: float32 [2048], replicated, may hold values from 0.1 to 1.9
- moe_in: bfloat16 [4096, 2048], P(('ep', 'tp')), may hold values from -6 to 6
- pre_gain: float32 [2048], replicated, may hold values from 0.1 to 1.9
- expert_ids: int32 [4096, 2], P(('ep', 'tp')), may hold values from 0 to 15, all different within a row; in each aligned block of 128 rows (0 to 127, 128 to 255, ...) at most 32 rows name the same one
- routed_expert_weight: float32 [4096, 2], P(('ep', 'tp')), may hold values from 0.2 to 1.5
- w_gate: bfloat16 [16, 2048, 768], P('ep', None, 'tp'), may hold values from -0.125 to 0.125
- w_up: bfloat16 [16, 2048, 768], P('ep', None, 'tp'), may hold values from -0.125 to 0.125
- w_down: bfloat16 [16, 768, 2048], P('ep', 'tp'), may hold values from -0.21875 to 0.21875
- common_expert_gate_weight: bfloat16 [2048, 512], P(None, 'tp'), may hold values from -0.125 to 0.125
- common_expert_up_weight: bfloat16 [2048, 512], P(None, 'tp'), may hold values from -0.125 to 0.125
- common_expert_down_weight: bfloat16 [512, 2048], P('tp'), may hold values from -0.25 to 0.25
- moe_gain: float32 [2048], replicated, may hold values from 0.1 to 1.9
Outputs:
- mixer_out: bfloat16 [8192, 2048], P(('ep', 'tp'))
- experts_out: bfloat16 [4096, 2048], P(('ep', 'tp'))
The draws below stay inside these ranges and needn't reach their ends.
Inputs may be any that keep to these rules, and one draw needn't show every extreme that they name: `expert_ids`: each row names 2 different experts; within the rows of one device no expert is named more than 32 times, and in every draw some expert is named exactly 32 times by the rows of some device.
All inputs are finite; a program needn't handle non-finite values.
Results may differ from the reference program's by a relative error of at most 0.012.
Values may be sent and summed in bfloat16 or wider, within the bound.
A program may use at most 128 MiB of HBM per device.

```python
import math
import jax
import jax.numpy as jnp
import numpy as np
from jax import lax

D = 2048
HEADS = 16
KV_HEADS = 4
HEAD_DIM = 64
WINDOW = 128
TOK_MOE = 128
TOPK = 2
FE = 768
SHARED = 512
EXPERTS = 16
CAP = 32
SEQ_ATT = 8192
TOKENS_MOE = 4096
N_EP = 8
N_TP = 4


def draw_att_queries(key, part):
    shape = (SEQ_ATT, KV_HEADS, HEADS // KV_HEADS, HEAD_DIM)
    base_draw = jax.random.truncated_normal(jax.random.fold_in(key, 21), -6.0, 6.0, shape, jnp.float32)
    return base_draw.reshape(SEQ_ATT, HEADS * HEAD_DIM).astype(jnp.bfloat16)


def draw_att_keys(key, part):
    shape = (SEQ_ATT, KV_HEADS, HEAD_DIM)
    base_draw = jax.random.truncated_normal(jax.random.fold_in(key, 31), -6.0, 6.0, shape, jnp.float32)
    return base_draw.reshape(SEQ_ATT, KV_HEADS * HEAD_DIM).astype(jnp.bfloat16)


def block_scale(stream_key, extent, cuts, least, largest):
    def one(dim, blocks):
        heights = jax.random.uniform(jax.random.fold_in(jax.random.fold_in(stream_key, 6), dim), (blocks,), jnp.float32, least / len(cuts), largest / len(cuts))
        return jnp.repeat(jnp.exp(heights), extent[dim] // blocks).reshape((-1,) + (1,) * (len(extent) - dim - 1))

    gain = one(*cuts[0])
    for cut in cuts[1:]:
        gain = gain * one(*cut)
    return gain


def deal_out(key, own, number, rows, amount, top, limit, lean):
    order = jax.random.permutation(key, amount)
    crowded, common = shares(amount, rows * top, limit, lean, True), shares(amount, rows * top, limit, lean, False)
    places = jnp.arange(amount)

    def named(tallies, rotation):
        used = int((tallies > 0).sum())
        fixed = max(1, used // 4)
        shifted = fixed + (places - fixed + rotation * (used - fixed)) % max(1, amount - fixed)
        return jnp.zeros((amount,), jnp.int32).at[order[jnp.where(places < fixed, places, shifted)]].set(jnp.asarray(tallies, jnp.int32))

    tallies = jnp.where(number % 4 == 0, named(crowded, number // 4), named(common, number - number // 4 - 1))
    mixed = jax.random.permutation(jax.random.fold_in(own, 3), amount)
    giver, taker = mixed[0:amount // 2 * 2:2], mixed[1:amount // 2 * 2:2]
    slack = jnp.minimum(tallies[giver] - 1, limit - tallies[taker]) // 2
    slack = jnp.where((giver == order[0]) | (taker == order[0]) | (tallies[taker] == 0), 0, jnp.maximum(slack, 0))
    shifted = jax.random.randint(jax.random.fold_in(own, 4), (amount // 2,), 0, 1 << 20) % (slack + 1)
    tallies = tallies.at[giver].add(-shifted).at[taker].add(shifted)
    members = jnp.searchsorted(jnp.cumsum(tallies), jnp.arange(rows * top), side="right").astype(jnp.int32)
    table = members.reshape(top, rows).T
    table = table[jax.random.permutation(jax.random.fold_in(own, 1), rows)]
    rotation = jax.random.randint(jax.random.fold_in(own, 2), (rows, 1), 0, top)
    return jnp.take_along_axis(table, (jnp.arange(top)[None, :] + rotation) % top, axis=1)


def shares(count, total, reach, lean, full):
    portions = [(1 << 20) // math.isqrt(rank ** lean) + 1 for rank in range(1, count + 1)]
    largest = reach if full else min(reach, max(-(-total // count), total * portions[0] // sum(portions)))
    least = 1 if total - largest >= count - 1 else 0
    given, rest = [largest] + [least] * (count - 1), total - largest - least * (count - 1)
    while rest > 0:
        free = [i for i in range(1, count) if given[i] < largest] or [i for i in range(1, count) if given[i] < reach]
        whole, budget = sum([portions[i] for i in free]), rest
        for i in free:
            more = min(reach - given[i], max(1, budget * portions[i] // whole), rest)
            given[i] = given[i] + more
            rest = rest - more
    return np.array(given)


def centred(stream_key, dims, width, reach, shards=(), kind=jnp.bfloat16):
    values = width * jax.random.normal(stream_key, dims, jnp.float32)
    if shards:
        values = values * block_scale(stream_key, dims, shards, -0.22, 0.18)
    return jnp.clip(values, -reach, reach).astype(kind)


def setup_inputs(seed: int = 0) -> dict:
    key_list = jax.random.split(jax.random.key(seed), 18)
    att_queries = draw_att_queries(jax.random.fold_in(key_list[17], 71), 0)
    att_keys = draw_att_keys(jax.random.fold_in(key_list[17], 71), 0)
    att_values = centred(key_list[2], (SEQ_ATT, KV_HEADS * HEAD_DIM), 1.0, 6.0, ((0, 32),))
    sink_logits = jnp.clip(jax.random.uniform(key_list[3], (HEADS,), jnp.float32, 3.0, 6.5), 3.0, 6.5)
    out_weight = centred(key_list[4], (HEADS * HEAD_DIM, D), (HEADS * HEAD_DIM) ** -0.5, 0.1875)
    att_gain = jnp.clip(1.0 + 0.18 * jax.random.normal(key_list[5], (D,), jnp.float32), 0.1, 1.9)
    moe_in = centred(key_list[6], (TOKENS_MOE, D), 1.0, 6.0, ((0, 32),))
    pre_gain = jnp.clip(1.0 + 0.18 * jax.random.normal(key_list[7], (D,), jnp.float32), 0.1, 1.9)
    expert_ids_keys = jax.random.split(jax.random.fold_in(key_list[8], 1), TOKENS_MOE // TOK_MOE)
    expert_ids_turns = jax.random.permutation(jax.random.fold_in(key_list[8], 3), TOKENS_MOE // TOK_MOE)
    expert_ids = jax.vmap(lambda own, number: deal_out(jax.random.fold_in(key_list[8], 2), own, number, TOK_MOE, EXPERTS, TOPK, CAP, 1))(expert_ids_keys, expert_ids_turns).reshape((TOKENS_MOE, TOPK))
    routed_expert_weight = jnp.clip(jnp.exp(math.log(1.5) - 2.014903 * jax.random.uniform(key_list[9], (TOKENS_MOE, TOPK), jnp.float32) ** block_scale(key_list[9], (TOKENS_MOE, TOPK), ((0, 32),), -0.2, 0.2)), 0.2, 1.5)
    w_gate = centred(key_list[10], (EXPERTS, D, FE), D ** -0.5, 0.125, ((0, 8), (2, 4)))
    w_up = centred(key_list[11], (EXPERTS, D, FE), D ** -0.5, 0.125, ((0, 8), (2, 4)))
    w_down = centred(key_list[12], (EXPERTS, FE, D), FE ** -0.5, 0.21875, ((0, 8), (1, 4)))
    common_expert_gate_weight = centred(key_list[13], (D, SHARED), D ** -0.5, 0.125, ((1, 4),))
    common_expert_up_weight = centred(key_list[14], (D, SHARED), D ** -0.5, 0.125, ((1, 4),))
    common_expert_down_weight = centred(key_list[15], (SHARED, D), SHARED ** -0.5, 0.25, ((0, 4),))
    moe_gain = jnp.clip(1.0 + 0.18 * jax.random.normal(key_list[16], (D,), jnp.float32), 0.1, 1.9)
    return {"att_queries": att_queries, "att_keys": att_keys, "att_values": att_values, "sink_logits": sink_logits, "out_weight": out_weight, "att_gain": att_gain, "moe_in": moe_in, "pre_gain": pre_gain, "expert_ids": expert_ids, "routed_expert_weight": routed_expert_weight, "w_gate": w_gate, "w_up": w_up, "w_down": w_down, "common_expert_gate_weight": common_expert_gate_weight, "common_expert_up_weight": common_expert_up_weight, "common_expert_down_weight": common_expert_down_weight, "moe_gain": moe_gain}


EPS = 1e-06
NEGATIVE = -1e+30

def rms_scale(inputs, gain_vec):
    mean_sq = lax.optimization_barrier(jnp.mean(inputs * inputs, axis=-1, keepdims=True))
    return inputs * lax.rsqrt(mean_sq + EPS) * gain_vec

def block_parts(hidden, down_rows, split_count):
    block_width = hidden.shape[-1] // split_count
    pieces = jnp.einsum('rbf,bfd->rbd', hidden.astype(jnp.float32).reshape(hidden.shape[0], split_count, block_width), down_rows.astype(jnp.float32).reshape(split_count, block_width, down_rows.shape[-1]))
    rounded = lax.optimization_barrier(pieces.astype(jnp.bfloat16))
    return lax.optimization_barrier(jnp.sum(rounded.astype(jnp.float32), axis=1))

def window_attention(att_queries, att_keys, att_values, sink_logits):
    group_size = HEADS // KV_HEADS
    blocks = SEQ_ATT // WINDOW
    padding = jnp.zeros((WINDOW, KV_HEADS * HEAD_DIM), att_keys.dtype)
    key_blocks = jnp.concatenate([padding, att_keys], axis=0).reshape(blocks + 1, WINDOW, KV_HEADS, HEAD_DIM)
    value_blocks = jnp.concatenate([padding, att_values], axis=0).reshape(blocks + 1, WINDOW, KV_HEADS, HEAD_DIM)
    query_blocks = att_queries.reshape(blocks, WINDOW, KV_HEADS, group_size, HEAD_DIM)
    distance = jnp.arange(WINDOW)[:, None] + WINDOW - jnp.arange(2 * WINDOW)[None, :]
    inside = (distance >= 0) & (distance < WINDOW)
    sink_grid = sink_logits.astype(jnp.float32).reshape(KV_HEADS, group_size)[:, :, None, None]
    score_scale = 1.0 / math.sqrt(HEAD_DIM)

    def one_block(block_index):
        key_band = lax.dynamic_slice_in_dim(key_blocks, block_index, 2, 0).reshape(2 * WINDOW, KV_HEADS, HEAD_DIM)
        value_band = lax.dynamic_slice_in_dim(value_blocks, block_index, 2, 0).reshape(2 * WINDOW, KV_HEADS, HEAD_DIM)
        query_block = lax.dynamic_index_in_dim(query_blocks, block_index, 0, keepdims=False)
        scores = jnp.einsum('qgjd,kgd->gjqk', query_block.astype(jnp.float32), key_band.astype(jnp.float32)) * score_scale
        key_pos = block_index * WINDOW - WINDOW + jnp.arange(2 * WINDOW)
        is_valid = inside & (key_pos >= 0)[None, :]
        scores = jnp.where(is_valid[None, None], scores, NEGATIVE)
        row_top = jnp.maximum(lax.optimization_barrier(jnp.max(scores, axis=-1, keepdims=True)), sink_grid)
        exp_scores = jnp.exp(scores - row_top)
        denominator = lax.optimization_barrier(jnp.sum(exp_scores, axis=-1, keepdims=True)) + jnp.exp(sink_grid - row_top)
        probs = (exp_scores / denominator).astype(jnp.bfloat16)
        head_mix = jnp.einsum('gjqk,kgd->qgjd', probs.astype(jnp.float32), value_band.astype(jnp.float32))
        return head_mix.astype(jnp.bfloat16).reshape(WINDOW, HEADS * HEAD_DIM)
    head_mix = lax.map(one_block, jnp.arange(blocks, dtype=jnp.int32))
    return head_mix.reshape(SEQ_ATT, HEADS * HEAD_DIM)

def routed_experts(normed, expert_ids, routed_expert_weight, w_gate, w_up, w_down):
    devices = N_EP * N_TP
    per_device = TOK_MOE * TOPK
    flat_ids = expert_ids.reshape(devices, per_device)
    earlier = jnp.arange(per_device)[None, :] < jnp.arange(per_device)[:, None]

    def positions_of(device_ids):
        return lax.optimization_barrier(jnp.sum((device_ids[:, None] == device_ids[None, :]) & earlier, axis=1)).astype(jnp.int32)
    position = lax.map(positions_of, flat_ids)
    device_index = jnp.arange(devices, dtype=jnp.int32)[:, None]
    slot_index = ((flat_ids * devices + device_index) * CAP + position).reshape(-1).astype(jnp.int32)
    token_index = (device_index * TOK_MOE + jnp.arange(per_device, dtype=jnp.int32)[None, :] // TOPK).reshape(-1)
    table_size = EXPERTS * devices * CAP
    row_table = jnp.zeros((table_size,), jnp.int32).at[slot_index].set(token_index.astype(jnp.int32))
    row_table = row_table.reshape(EXPERTS, devices * CAP)
    weight_table = jnp.zeros((table_size,), jnp.float32).at[slot_index].set(routed_expert_weight.reshape(-1))
    weight_table = weight_table.reshape(EXPERTS, devices * CAP)

    def add_expert(running, expert_index):
        row_ids = lax.dynamic_index_in_dim(row_table, expert_index, 0, keepdims=False)
        slot_weights = lax.dynamic_index_in_dim(weight_table, expert_index, 0, keepdims=False)
        picked = normed[row_ids]
        gate_act = jnp.dot(picked, w_gate[expert_index], preferred_element_type=jnp.float32)
        up_act = jnp.dot(picked, w_up[expert_index], preferred_element_type=jnp.float32)
        hidden = (jax.nn.silu(gate_act) * up_act).astype(jnp.bfloat16)
        output = block_parts(hidden, w_down[expert_index], N_TP).astype(jnp.bfloat16)
        running = running.at[row_ids].add(slot_weights[:, None] * output.astype(jnp.float32))
        return (running, None)
    start_value = jnp.zeros((TOKENS_MOE, D), jnp.float32)
    return lax.scan(add_expert, start_value, jnp.arange(EXPERTS, dtype=jnp.int32))[0]

def reference(att_queries, att_keys, att_values, sink_logits, out_weight, att_gain, moe_in, pre_gain, expert_ids, routed_expert_weight, w_gate, w_up, w_down, common_expert_gate_weight, common_expert_up_weight, common_expert_down_weight, moe_gain):
    head_mix = window_attention(att_queries, att_keys, att_values, sink_logits)
    projected = jnp.dot(head_mix, out_weight, preferred_element_type=jnp.float32)
    mixer_out = rms_scale(projected, att_gain).astype(jnp.bfloat16)
    normed = rms_scale(moe_in.astype(jnp.float32), pre_gain).astype(jnp.bfloat16)
    routed = routed_experts(normed, expert_ids, routed_expert_weight, w_gate, w_up, w_down)

    def shared_rows(row_block):
        gate_act = jnp.dot(row_block, common_expert_gate_weight, preferred_element_type=jnp.float32)
        up_act = jnp.dot(row_block, common_expert_up_weight, preferred_element_type=jnp.float32)
        common_expert_hidden = (jax.nn.silu(gate_act) * up_act).astype(jnp.bfloat16)
        return block_parts(common_expert_hidden, common_expert_down_weight, N_TP)
    shared_sum = lax.map(shared_rows, normed.reshape(N_EP * N_TP, TOK_MOE, D)).reshape(TOKENS_MOE, D)
    combined = routed + shared_sum
    experts_out = rms_scale(combined, moe_gain).astype(jnp.bfloat16)
    return (mixer_out, experts_out)
```

```python
import functools
import math

import jax
import jax.numpy as jnp
from jax import lax
from jax.experimental import pallas as pl
from jax.experimental.pallas import tpu as pltpu
from jax.sharding import PartitionSpec as P

HEADS = 16
KV_HEADS = 4
HEAD_DIM = 64
WINDOW = 128

EPS = 1e-06
NEGATIVE = -1e30

VMEM = pl.BlockSpec(memory_space=pltpu.VMEM)
SMEM = pl.BlockSpec(memory_space=pltpu.SMEM)
ANY = pl.BlockSpec(memory_space=pl.ANY)
F32 = jnp.float32
BF16 = jnp.bfloat16


def iota(shape, dim):
    return lax.broadcasted_iota(jnp.int32, shape, dim)


def params():
    return pltpu.CompilerParams(vmem_limit_bytes=56 * 1024 * 1024)


def rms_scale(inputs, gain_vec):
    mean_sq = jnp.mean(inputs * inputs, axis=-1, keepdims=True)
    return inputs * lax.rsqrt(mean_sq + EPS) * gain_vec


def attention_kernel(
    start_ref, sink_ref, q_ref, k_ref, v_ref, rim_ref, w_hbm, gain_ref, out_ref, w_vmem, mix, sem
):
    load = pltpu.make_async_copy(w_hbm, w_vmem, sem)
    load.start()
    group_size = HEADS // KV_HEADS
    blocks = q_ref.shape[0] // WINDOW
    kv_width = KV_HEADS * HEAD_DIM
    shape = (WINDOW, 2 * WINDOW)
    gap = iota(shape, 0) + WINDOW - iota(shape, 1)
    inside = (gap >= 0) & (gap < WINDOW)
    for n in range(blocks):
        rows = pl.ds(n * WINDOW, WINDOW)
        if n == 0:
            valid = inside & (iota(shape, 1) + start_ref[0] >= WINDOW)
        else:
            valid = inside
        for g in range(KV_HEADS):
            cols = pl.ds(g * HEAD_DIM, HEAD_DIM)
            if n == 0:
                keys = jnp.concatenate([rim_ref[:, cols], k_ref[rows, cols]], axis=0)
                rim_cols = pl.ds(kv_width + g * HEAD_DIM, HEAD_DIM)
                values = jnp.concatenate([rim_ref[:, rim_cols], v_ref[rows, cols]], axis=0)
            else:
                band = pl.ds((n - 1) * WINDOW, 2 * WINDOW)
                keys, values = k_ref[band, cols], v_ref[band, cols]
            mixed = []
            for j in range(group_size):
                h = g * group_size + j
                query = q_ref[rows, pl.ds(h * HEAD_DIM, HEAD_DIM)]
                scores = lax.dot_general(
                    query, keys, (((1,), (1,)), ((), ())), preferred_element_type=F32
                ) * (1.0 / math.sqrt(HEAD_DIM))
                scores = jnp.where(valid, scores, NEGATIVE)
                sink = sink_ref[h]
                top = jnp.maximum(jnp.max(scores, axis=-1, keepdims=True), sink)
                weights = jnp.exp(scores - top)
                total = jnp.sum(weights, axis=-1, keepdims=True) + jnp.exp(sink - top)
                probs = (weights * (1.0 / total)).astype(BF16)
                mixed.append(jnp.dot(probs, values, preferred_element_type=F32).astype(BF16))
            width = group_size * HEAD_DIM
            mix[rows, pl.ds(g * width, width)] = jnp.concatenate(mixed, axis=1)
    load.wait()
    for n in range(blocks):
        rows = pl.ds(n * WINDOW, WINDOW)
        projected = jnp.dot(mix[rows, :], w_vmem[...], preferred_element_type=F32)
        out_ref[rows, :] = rms_scale(projected, gain_ref[...]).astype(BF16)


def attention(att_queries, att_keys, att_values, rim, sink_logits, out_weight, att_gain, start):
    rows, width = att_queries.shape
    d = out_weight.shape[1]
    return pl.pallas_call(
        attention_kernel,
        out_shape=jax.ShapeDtypeStruct((rows, d), BF16),
        in_specs=[SMEM, SMEM, VMEM, VMEM, VMEM, VMEM, ANY, VMEM],
        out_specs=VMEM,
        scratch_shapes=[
            pltpu.VMEM(out_weight.shape, BF16),
            pltpu.VMEM((rows, width), BF16),
            pltpu.SemaphoreType.DMA,
        ],
        compiler_params=params(),
        cost_estimate=pl.CostEstimate(
            flops=12_000_000_000, bytes_accessed=8_000_000, transcendentals=2_000_000
        ),
        name="attention",
    )(start, sink_logits, att_queries, att_keys, att_values, rim, out_weight, att_gain[None])


def pack_kernel(slot_cap, experts, ids_ref, x_ref, gain_ref, normed_ref, packed_ref):
    tokens = x_ref.shape[0]
    slots = packed_ref.shape[0]
    normed = rms_scale(x_ref[...].astype(F32), gain_ref[...]).astype(BF16)
    normed_ref[...] = normed
    numbers = iota((experts, tokens), 0)
    hit = numbers == ids_ref[0:1, :]
    for k in range(1, ids_ref.shape[0]):
        hit = hit | (numbers == ids_ref[k : k + 1, :])
    earlier = (iota((tokens, tokens), 0) < iota((tokens, tokens), 1)).astype(F32).astype(BF16)
    before = jnp.dot(hit.astype(F32).astype(BF16), earlier, preferred_element_type=F32)
    place = jnp.where(hit, before + 1.0, 0.0).astype(BF16)
    from_slot = iota((slots, experts), 0) - iota((slots, experts), 1) * slot_cap
    spread = ((from_slot >= 0) & (from_slot < slot_cap)).astype(F32).astype(BF16)
    wanted = lax.rem(iota((slots, tokens), 0), slot_cap).astype(F32) + 1.0
    chosen = jnp.dot(spread, place, preferred_element_type=F32) == wanted
    chosen = chosen.astype(F32).astype(BF16)
    step = slots // 4
    for i in range(4):
        packed_ref[i * step : (i + 1) * step, :] = jnp.dot(
            chosen[i * step : (i + 1) * step], normed, preferred_element_type=F32
        ).astype(BF16)


def pack(moe_in, pre_gain, expert_ids, slot_cap, experts):
    tokens, d = moe_in.shape
    return pl.pallas_call(
        functools.partial(pack_kernel, slot_cap, experts),
        out_shape=(
            jax.ShapeDtypeStruct((tokens, d), BF16),
            jax.ShapeDtypeStruct((slot_cap * experts, d), BF16),
        ),
        in_specs=[VMEM] * 3,
        out_specs=(VMEM, VMEM),
        compiler_params=params(),
        cost_estimate=pl.CostEstimate(
            flops=2_000_000_000, bytes_accessed=4_000_000, transcendentals=0
        ),
        name="pack",
    )(expert_ids.T, moe_in, pre_gain[None])


def mlp_kernel(blocks, rows_ref, *refs):
    gates, ups, downs = (refs[i * blocks : (i + 1) * blocks] for i in range(3))
    out_ref, g_vmem, u_vmem, d_vmem, hidden, sems = refs[3 * blocks :]
    width = g_vmem.shape[2]
    loads = []
    for b in range(blocks):
        loads.append(pltpu.make_async_copy(gates[b], g_vmem.at[b], sems.at[b]))
        loads.append(pltpu.make_async_copy(ups[b], u_vmem.at[b], sems.at[blocks + b]))
    for b in range(blocks):
        slot = d_vmem.at[pl.ds(b * width, width)]
        loads.append(pltpu.make_async_copy(downs[b], slot, sems.at[2 * blocks + b]))
    for load in loads:
        load.start()
    total = rows_ref.shape[0]
    tile = min(total, 256)
    tiles = total // tile
    for b in range(blocks):
        loads[2 * b].wait()
        loads[2 * b + 1].wait()

        @pl.loop(0, tiles)
        def _(i):
            rows = pl.ds(pl.multiple_of(i * tile, tile), tile)
            gate = jnp.dot(rows_ref[rows, :], g_vmem[b], preferred_element_type=F32)
            up = jnp.dot(rows_ref[rows, :], u_vmem[b], preferred_element_type=F32)
            hidden[b, rows, :] = (gate / (1.0 + jnp.exp(-gate)) * up).astype(BF16)

    for load in loads[2 * blocks :]:
        load.wait()

    @pl.loop(0, tiles)
    def _(i):
        rows = pl.ds(pl.multiple_of(i * tile, tile), tile)
        units = jnp.concatenate([hidden[b, rows, :] for b in range(blocks)], axis=1)
        out_ref[rows, :] = jnp.dot(units, d_vmem[...], preferred_element_type=F32).astype(
            out_ref.dtype
        )


def mlp(rows, gates, ups, downs, dtype, name):
    total, d = rows.shape
    blocks = len(gates)
    width = gates[0].shape[1]
    return pl.pallas_call(
        functools.partial(mlp_kernel, blocks),
        out_shape=jax.ShapeDtypeStruct((total, d), dtype),
        in_specs=[VMEM] + [ANY] * (3 * blocks),
        out_specs=VMEM,
        scratch_shapes=[
            pltpu.VMEM((blocks, d, width), BF16),
            pltpu.VMEM((blocks, d, width), BF16),
            pltpu.VMEM((blocks * width, d), BF16),
            pltpu.VMEM((blocks, total, width), BF16),
            pltpu.SemaphoreType.DMA((3 * blocks,)),
        ],
        compiler_params=params(),
        cost_estimate=pl.CostEstimate(
            flops=6 * total * d * width * blocks,
            bytes_accessed=6 * d * width * blocks + 4 * total * d,
            transcendentals=total * width * blocks,
        ),
        name=name,
    )(rows, *gates, *ups, *downs)


def combine_kernel(
    slot_cap, experts, ids_ref, weight_ref, returned_ref, shared_ref, gain_ref, out_ref
):
    tokens, top_count = ids_ref.shape
    slots = returned_ref.shape[0]
    numbers = iota((tokens, experts), 1)
    hits = [numbers == ids_ref[:, k : k + 1] for k in range(top_count)]
    hit = functools.reduce(lambda a, b: a | b, hits)
    earlier = (iota((tokens, tokens), 0) > iota((tokens, tokens), 1)).astype(F32).astype(BF16)
    before = jnp.dot(earlier, hit.astype(F32).astype(BF16), preferred_element_type=F32)
    slot_of = before + (numbers * slot_cap).astype(F32)
    lanes = iota((tokens, slots), 1).astype(F32)
    combined = shared_ref[...]
    for k in range(top_count):
        slot = jnp.sum(jnp.where(hits[k], slot_of, 0.0), axis=1, keepdims=True)
        chosen = (lanes == slot).astype(F32).astype(BF16)
        picked = jnp.dot(chosen, returned_ref[...], preferred_element_type=F32)
        combined = combined + weight_ref[:, k : k + 1] * picked
    out_ref[...] = rms_scale(combined, gain_ref[...]).astype(BF16)


def combine(expert_ids, routed_expert_weight, returned, shared_sum, moe_gain, slot_cap, experts):
    return pl.pallas_call(
        functools.partial(combine_kernel, slot_cap, experts),
        out_shape=jax.ShapeDtypeStruct(shared_sum.shape, BF16),
        in_specs=[VMEM] * 5,
        out_specs=VMEM,
        compiler_params=params(),
        cost_estimate=pl.CostEstimate(
            flops=2_000_000_000, bytes_accessed=4_000_000, transcendentals=0
        ),
        name="combine",
    )(expert_ids, routed_expert_weight, returned, shared_sum, moe_gain[None])


def swap(array, distance):
    size = lax.axis_size("tp")
    return lax.ppermute(array, "tp", [(i, i ^ distance) for i in range(size)])


def doubled(held, distance):
    while distance >= 1:
        held = held + [swap(block, distance) for block in held]
        distance //= 2
    return held


def whole_expert(stacked):
    held = [stacked]
    distance = lax.axis_size("tp") // 2
    here = lax.axis_index("tp")
    while held[0].shape[0] > 1:
        half = held[0].shape[0] // 2
        bit = (here // distance) % 2
        kept = [lax.dynamic_slice_in_dim(block, bit * half, half, 0) for block in held]
        sent = [lax.dynamic_slice_in_dim(block, (1 - bit) * half, half, 0) for block in held]
        held = kept + [swap(block, distance) for block in sent]
        distance //= 2
    return doubled([block[0] for block in held], distance)


def body(
    att_queries,
    att_keys,
    att_values,
    sink_logits,
    out_weight,
    att_gain,
    moe_in,
    pre_gain,
    expert_ids,
    routed_expert_weight,
    w_gate,
    w_up,
    w_down,
    common_expert_gate_weight,
    common_expert_up_weight,
    common_expert_down_weight,
    moe_gain,
):
    devices = lax.axis_size(("ep", "tp"))
    tok_rows = att_queries.shape[0]
    tokens = moe_in.shape[0]
    top_count = expert_ids.shape[1]
    experts = w_gate.shape[0] * lax.axis_size("ep")
    slot_cap = 2 * tokens * top_count // experts

    normed, packed = pack(moe_in, pre_gain, expert_ids, slot_cap, experts)
    arrived = lax.all_to_all(packed, ("ep", "tp"), split_axis=0, concat_axis=0, tiled=True)

    gates, ups, downs = whole_expert(w_gate), whole_expert(w_up), whole_expert(w_down)
    half = lax.axis_size("tp") // 2
    common_gates = doubled([common_expert_gate_weight], half)
    common_ups = doubled([common_expert_up_weight], half)
    common_downs = doubled([common_expert_down_weight], half)

    edge = tok_rows - WINDOW
    rim = lax.ppermute(
        jnp.concatenate([att_keys[edge:], att_values[edge:]], axis=1),
        ("ep", "tp"),
        [(i, i + 1) for i in range(devices - 1)],
    )
    start = (lax.axis_index(("ep", "tp")) * tok_rows).astype(jnp.int32).reshape(1)
    mixer_out = attention(
        att_queries, att_keys, att_values, rim, sink_logits, out_weight, att_gain, start
    )

    outputs = mlp(arrived, gates, ups, downs, BF16, "expert")
    returned = lax.all_to_all(outputs, ("ep", "tp"), split_axis=0, concat_axis=0, tiled=True)
    shared_sum = mlp(normed, common_gates, common_ups, common_downs, F32, "shared")
    experts_out = combine(
        expert_ids, routed_expert_weight, returned, shared_sum, moe_gain, slot_cap, experts
    )
    return (mixer_out, experts_out)


def solution(mesh):
    in_specs = (
        P(("ep", "tp"), None),
        P(("ep", "tp"), None),
        P(("ep", "tp"), None),
        P(),
        P(),
        P(),
        P(("ep", "tp"), None),
        P(),
        P(("ep", "tp"), None),
        P(("ep", "tp"), None),
        P("ep", None, "tp"),
        P("ep", None, "tp"),
        P("ep", "tp", None),
        P(None, "tp"),
        P(None, "tp"),
        P("tp", None),
        P(),
    )
    out_specs = (P(("ep", "tp"), None), P(("ep", "tp"), None))
    return jax.shard_map(body, mesh=mesh, in_specs=in_specs, out_specs=out_specs, check_vma=False)
```

```python
import functools
import math

import jax
import jax.numpy as jnp
from jax import lax
from jax.experimental import pallas as pl
from jax.experimental.pallas import tpu as pltpu
from jax.sharding import PartitionSpec as P

HEADS = 16
KV_HEADS = 4
HEAD_DIM = 64
WINDOW = 128

EPS = 1e-06
NEGATIVE = -1e30
PLANES = 2

VMEM = pl.BlockSpec(memory_space=pltpu.VMEM)
SMEM = pl.BlockSpec(memory_space=pltpu.SMEM)
ANY = pl.BlockSpec(memory_space=pl.ANY)
F32 = jnp.float32
BF16 = jnp.bfloat16


def iota(shape, dim):
    return lax.broadcasted_iota(jnp.int32, shape, dim)


def params():
    return pltpu.CompilerParams(vmem_limit_bytes=56 * 1024 * 1024)


def rms_scale(inputs, gain_vec):
    mean_sq = jnp.mean(inputs * inputs, axis=-1, keepdims=True)
    return inputs * lax.rsqrt(mean_sq + EPS) * gain_vec


def attention_kernel(
    start_ref, sink_ref, q_ref, k_ref, v_ref, rim_ref, w_hbm, gain_ref, out_ref, w_vmem, mix, sem
):
    load = pltpu.make_async_copy(w_hbm, w_vmem, sem)
    load.start()
    group_size = HEADS // KV_HEADS
    blocks = q_ref.shape[0] // WINDOW
    kv_width = KV_HEADS * HEAD_DIM
    shape = (WINDOW, 2 * WINDOW)
    gap = iota(shape, 0) + WINDOW - iota(shape, 1)
    inside = (gap >= 0) & (gap < WINDOW)
    for n in range(blocks):
        rows = pl.ds(n * WINDOW, WINDOW)
        if n == 0:
            valid = inside & (iota(shape, 1) + start_ref[0] >= WINDOW)
        else:
            valid = inside
        for g in range(KV_HEADS):
            cols = pl.ds(g * HEAD_DIM, HEAD_DIM)
            if n == 0:
                keys = jnp.concatenate([rim_ref[:, cols], k_ref[rows, cols]], axis=0)
                rim_cols = pl.ds(kv_width + g * HEAD_DIM, HEAD_DIM)
                values = jnp.concatenate([rim_ref[:, rim_cols], v_ref[rows, cols]], axis=0)
            else:
                band = pl.ds((n - 1) * WINDOW, 2 * WINDOW)
                keys, values = k_ref[band, cols], v_ref[band, cols]
            mixed = []
            for j in range(group_size):
                h = g * group_size + j
                query = q_ref[rows, pl.ds(h * HEAD_DIM, HEAD_DIM)]
                scores = lax.dot_general(
                    query, keys, (((1,), (1,)), ((), ())), preferred_element_type=F32
                ) * (1.0 / math.sqrt(HEAD_DIM))
                scores = jnp.where(valid, scores, NEGATIVE)
                sink = sink_ref[h]
                top = jnp.maximum(jnp.max(scores, axis=-1, keepdims=True), sink)
                weights = jnp.exp(scores - top)
                total = jnp.sum(weights, axis=-1, keepdims=True) + jnp.exp(sink - top)
                probs = (weights * (1.0 / total)).astype(BF16)
                mixed.append(jnp.dot(probs, values, preferred_element_type=F32).astype(BF16))
            width = group_size * HEAD_DIM
            mix[rows, pl.ds(g * width, width)] = jnp.concatenate(mixed, axis=1)
    load.wait()
    for n in range(blocks):
        rows = pl.ds(n * WINDOW, WINDOW)
        projected = jnp.dot(mix[rows, :], w_vmem[...], preferred_element_type=F32)
        out_ref[rows, :] = rms_scale(projected, gain_ref[...]).astype(BF16)


def attention(att_queries, att_keys, att_values, rim, sink_logits, out_weight, att_gain, start):
    rows, width = att_queries.shape
    d = out_weight.shape[1]
    return pl.pallas_call(
        attention_kernel,
        out_shape=jax.ShapeDtypeStruct((rows, d), BF16),
        in_specs=[SMEM, SMEM, VMEM, VMEM, VMEM, VMEM, ANY, VMEM],
        out_specs=VMEM,
        scratch_shapes=[
            pltpu.VMEM(out_weight.shape, BF16),
            pltpu.VMEM((rows, width), BF16),
            pltpu.SemaphoreType.DMA,
        ],
        compiler_params=params(),
        cost_estimate=pl.CostEstimate(
            flops=12_000_000_000, bytes_accessed=8_000_000, transcendentals=2_000_000
        ),
        name="attention",
    )(start, sink_logits, att_queries, att_keys, att_values, rim, out_weight, att_gain[None])


def pack_block(slot_cap, plane, ids_ref, normed, packed_ref):
    tokens = normed.shape[0]
    slots = packed_ref.shape[0]
    groups = slots // slot_cap
    numbers = iota((groups, tokens), 0) * PLANES + plane
    hit = numbers == ids_ref[0:1, :]
    for k in range(1, ids_ref.shape[0]):
        hit = hit | (numbers == ids_ref[k : k + 1, :])
    earlier = (iota((tokens, tokens), 0) < iota((tokens, tokens), 1)).astype(F32).astype(BF16)
    before = jnp.dot(hit.astype(F32).astype(BF16), earlier, preferred_element_type=F32)
    place = jnp.where(hit, before + 1.0, 0.0).astype(BF16)
    from_slot = iota((slots, groups), 0) - iota((slots, groups), 1) * slot_cap
    spread = ((from_slot >= 0) & (from_slot < slot_cap)).astype(F32).astype(BF16)
    wanted = lax.rem(iota((slots, tokens), 0), slot_cap).astype(F32) + 1.0
    chosen = jnp.dot(spread, place, preferred_element_type=F32) == wanted
    chosen = chosen.astype(F32).astype(BF16)
    step = slots // 2
    for i in range(2):
        packed_ref[i * step : (i + 1) * step, :] = jnp.dot(
            chosen[i * step : (i + 1) * step], normed, preferred_element_type=F32
        ).astype(BF16)


def norm_pack_kernel(slot_cap, plane_ref, ids_ref, x_ref, gain_ref, normed_ref, packed_ref):
    normed = rms_scale(x_ref[...].astype(F32), gain_ref[...]).astype(BF16)
    normed_ref[...] = normed
    pack_block(slot_cap, plane_ref[0], ids_ref, normed, packed_ref)


def pack_kernel(slot_cap, plane_ref, ids_ref, normed_ref, packed_ref):
    pack_block(slot_cap, plane_ref[0], ids_ref, normed_ref[...], packed_ref)


def small_cost(flops=1_000_000_000):
    return pl.CostEstimate(flops=flops, bytes_accessed=2_000_000, transcendentals=0)


def norm_pack(moe_in, pre_gain, ids_t, plane, slot_cap, slots):
    tokens, d = moe_in.shape
    return pl.pallas_call(
        functools.partial(norm_pack_kernel, slot_cap),
        out_shape=(
            jax.ShapeDtypeStruct((tokens, d), BF16),
            jax.ShapeDtypeStruct((slots, d), BF16),
        ),
        in_specs=[SMEM] + [VMEM] * 3,
        out_specs=(VMEM, VMEM),
        compiler_params=params(),
        cost_estimate=small_cost(),
        name="norm_pack",
    )(plane, ids_t, moe_in, pre_gain[None])


def pack(normed, ids_t, plane, slot_cap, slots):
    return pl.pallas_call(
        functools.partial(pack_kernel, slot_cap),
        out_shape=jax.ShapeDtypeStruct((slots, normed.shape[1]), BF16),
        in_specs=[SMEM] + [VMEM] * 2,
        out_specs=VMEM,
        compiler_params=params(),
        cost_estimate=small_cost(),
        name="pack",
    )(plane, ids_t, normed)


def mlp_kernel(blocks, inputs, transposed, *refs):
    rows_refs, refs = refs[:inputs], refs[inputs:]
    gates, ups, downs = (refs[i * blocks : (i + 1) * blocks] for i in range(3))
    refs = refs[3 * blocks :]
    out_refs, refs = refs[:inputs], refs[inputs:]
    g_vmem, u_vmem, d_vmem, hidden, sems = refs
    width = d_vmem.shape[0] // blocks
    loads = []
    for b in range(blocks):
        loads.append(pltpu.make_async_copy(gates[b], g_vmem.at[b], sems.at[b]))
        loads.append(pltpu.make_async_copy(ups[b], u_vmem.at[b], sems.at[blocks + b]))
    for b in range(blocks):
        slot = d_vmem.at[pl.ds(b * width, width)]
        loads.append(pltpu.make_async_copy(downs[b], slot, sems.at[2 * blocks + b]))
    for load in loads:
        load.start()
    dims = (((1,), (1 if transposed else 0,)), ((), ()))
    total = rows_refs[0].shape[0]
    for b in range(blocks):
        loads[2 * b].wait()
        loads[2 * b + 1].wait()
        for i in range(inputs):
            rows = rows_refs[i][...]
            gate = lax.dot_general(rows, g_vmem[b], dims, preferred_element_type=F32)
            up = lax.dot_general(rows, u_vmem[b], dims, preferred_element_type=F32)
            hidden[b, i * total : (i + 1) * total, :] = (
                gate / (1.0 + jnp.exp(-gate)) * up
            ).astype(BF16)
    for load in loads[2 * blocks :]:
        load.wait()
    for i in range(inputs):
        units = jnp.concatenate(
            [hidden[b, i * total : (i + 1) * total, :] for b in range(blocks)], axis=1
        )
        out_refs[i][...] = jnp.dot(units, d_vmem[...], preferred_element_type=F32).astype(
            out_refs[i].dtype
        )


def mlp(rows, gates, ups, downs, transposed, dtype, name):
    total, d = rows[0].shape
    blocks, inputs = len(gates), len(rows)
    width = downs[0].shape[0]
    all_rows = total * inputs
    return pl.pallas_call(
        functools.partial(mlp_kernel, blocks, inputs, transposed),
        out_shape=[jax.ShapeDtypeStruct((total, d), dtype)] * inputs,
        in_specs=[VMEM] * inputs + [ANY] * (3 * blocks),
        out_specs=[VMEM] * inputs,
        scratch_shapes=[
            pltpu.VMEM((blocks,) + gates[0].shape, BF16),
            pltpu.VMEM((blocks,) + gates[0].shape, BF16),
            pltpu.VMEM((blocks * width, d), BF16),
            pltpu.VMEM((blocks, all_rows, width), BF16),
            pltpu.SemaphoreType.DMA((3 * blocks,)),
        ],
        compiler_params=params(),
        cost_estimate=pl.CostEstimate(
            flops=6 * all_rows * d * width * blocks,
            bytes_accessed=6 * d * width * blocks + 4 * all_rows * d,
            transcendentals=all_rows * width * blocks,
        ),
        name=name,
    )(*rows, *gates, *ups, *downs)


def partial_sum(slot_cap, plane, ids_ref, weight_ref, returned_ref, shared_ref):
    tokens, top_count = ids_ref.shape
    slots = returned_ref.shape[0]
    groups = slots // slot_cap
    index = iota((tokens, groups), 1)
    hits = [index * PLANES + plane == ids_ref[:, k : k + 1] for k in range(top_count)]
    hit = functools.reduce(lambda a, b: a | b, hits)
    earlier = (iota((tokens, tokens), 0) > iota((tokens, tokens), 1)).astype(F32).astype(BF16)
    before = jnp.dot(earlier, hit.astype(F32).astype(BF16), preferred_element_type=F32)
    place = before + (index * slot_cap + 1).astype(F32)
    lanes = iota((tokens, slots), 1).astype(F32) + 1.0
    combined = shared_ref[...]
    for k in range(top_count):
        slot = jnp.sum(jnp.where(hits[k], place, 0.0), axis=1, keepdims=True)
        chosen = (lanes == slot).astype(F32).astype(BF16)
        picked = jnp.dot(chosen, returned_ref[...], preferred_element_type=F32)
        combined = combined + weight_ref[:, k : k + 1] * picked
    return combined


def part_kernel(slot_cap, plane_ref, ids_ref, weight_ref, returned_ref, shared_ref, out_ref):
    out_ref[...] = partial_sum(
        slot_cap, plane_ref[0], ids_ref, weight_ref, returned_ref, shared_ref
    ).astype(BF16)


def final_kernel(
    slot_cap,
    plane_ref,
    ids_ref,
    weight_ref,
    returned_ref,
    shared_ref,
    other_ref,
    gain_ref,
    out_ref,
):
    combined = partial_sum(slot_cap, plane_ref[0], ids_ref, weight_ref, returned_ref, shared_ref)
    combined = combined + other_ref[...].astype(F32)
    out_ref[...] = rms_scale(combined, gain_ref[...]).astype(BF16)


def combine(kernel, name, slot_cap, plane, *arrays):
    return pl.pallas_call(
        functools.partial(kernel, slot_cap),
        out_shape=jax.ShapeDtypeStruct(arrays[3].shape, BF16),
        in_specs=[SMEM] + [VMEM] * len(arrays),
        out_specs=VMEM,
        compiler_params=params(),
        cost_estimate=small_cost(),
        name=name,
    )(plane, *arrays)


def swap(array, distance):
    size = lax.axis_size("tp")
    return lax.ppermute(array, "tp", [(i, i ^ distance) for i in range(size)])


def doubled(held, distance):
    while distance >= 1:
        held = held + [swap(block, distance) for block in held]
        distance //= 2
    return held


def one_expert(stacked, plane, far):
    kept = lax.dynamic_index_in_dim(stacked, plane, 0, keepdims=False)
    sent = lax.dynamic_index_in_dim(stacked, 1 - plane, 0, keepdims=False)
    return doubled([kept, swap(sent, far)], far // 2)


def exchange(array):
    return lax.all_to_all(array, "ep", split_axis=0, concat_axis=0, tiled=True)


def body(
    att_queries,
    att_keys,
    att_values,
    sink_logits,
    out_weight,
    att_gain,
    moe_in,
    pre_gain,
    expert_ids,
    routed_expert_weight,
    w_gate,
    w_up,
    w_down,
    common_expert_gate_weight,
    common_expert_up_weight,
    common_expert_down_weight,
    moe_gain,
):
    assert w_gate.shape[0] == PLANES
    devices = lax.axis_size(("ep", "tp"))
    tok_rows = att_queries.shape[0]
    tokens = moe_in.shape[0]
    top_count = expert_ids.shape[1]
    groups = lax.axis_size("ep")
    slot_cap = 2 * tokens * top_count // (PLANES * groups)
    slots = slot_cap * groups
    far = lax.axis_size("tp") // PLANES
    plane = (lax.axis_index("tp") // far).astype(jnp.int32)
    plane_arg = plane.reshape(1)

    edge = tok_rows - WINDOW
    rim = lax.ppermute(
        jnp.concatenate([att_keys[edge:], att_values[edge:]], axis=1),
        ("ep", "tp"),
        [(i, i + 1) for i in range(devices - 1)],
    )
    far_ids = swap(expert_ids, far)
    far_weight = swap(routed_expert_weight, far)

    normed, packed = norm_pack(moe_in, pre_gain, expert_ids.T, plane_arg, slot_cap, slots)
    far_normed = swap(normed, far)
    arrived = exchange(packed)
    far_packed = pack(far_normed, far_ids.T, plane_arg, slot_cap, slots)
    far_arrived = exchange(far_packed)

    gates = one_expert(jnp.swapaxes(w_gate, 1, 2), plane, far)
    w_up, w_down, far_normed = lax.optimization_barrier((w_up, w_down, far_normed))
    ups = one_expert(jnp.swapaxes(w_up, 1, 2), plane, far)
    downs = one_expert(w_down, plane, far)
    common_gates = doubled([common_expert_gate_weight], far // 2)
    common_ups = doubled([common_expert_up_weight], far // 2)
    common_downs = doubled([common_expert_down_weight], far // 2)

    start = (lax.axis_index(("ep", "tp")) * tok_rows).astype(jnp.int32).reshape(1)
    mixer_out = attention(
        att_queries, att_keys, att_values, rim, sink_logits, out_weight, att_gain, start
    )
    shared_own, shared_far = mlp(
        [normed, far_normed], common_gates, common_ups, common_downs, False, F32, "shared"
    )
    far_arrived, arrived, mixer_out, shared_own, shared_far = lax.optimization_barrier(
        (far_arrived, arrived, mixer_out, shared_own, shared_far)
    )

    (far_outputs,) = mlp([far_arrived], gates, ups, downs, True, BF16, "far_expert")
    far_returned = exchange(far_outputs)
    (outputs,) = mlp([arrived], gates, ups, downs, True, BF16, "own_expert")
    returned = exchange(outputs)
    far_part = combine(
        part_kernel, "far_part", slot_cap, plane_arg, far_ids, far_weight, far_returned, shared_far
    )
    other = swap(far_part, far)
    experts_out = combine(
        final_kernel,
        "final",
        slot_cap,
        plane_arg,
        expert_ids,
        routed_expert_weight,
        returned,
        shared_own,
        other,
        moe_gain[None],
    )
    return (mixer_out, experts_out)


def solution(mesh):
    in_specs = (
        P(("ep", "tp"), None),
        P(("ep", "tp"), None),
        P(("ep", "tp"), None),
        P(),
        P(),
        P(),
        P(("ep", "tp"), None),
        P(),
        P(("ep", "tp"), None),
        P(("ep", "tp"), None),
        P("ep", None, "tp"),
        P("ep", None, "tp"),
        P("ep", "tp", None),
        P(None, "tp"),
        P(None, "tp"),
        P("tp", None),
        P(),
    )
    out_specs = (P(("ep", "tp"), None), P(("ep", "tp"), None))
    return jax.shard_map(body, mesh=mesh, in_specs=in_specs, out_specs=out_specs, check_vma=False)
```

```python
import functools
import math

import jax
import jax.numpy as jnp
from jax import lax
from jax.experimental import pallas as pl
from jax.experimental.pallas import tpu as pltpu
from jax.sharding import PartitionSpec as P

HEADS = 16
KV_HEADS = 4
HEAD_DIM = 64
WINDOW = 128

EPS = 1e-06
NEGATIVE = -1e30
PLANES = 2

VMEM = pl.BlockSpec(memory_space=pltpu.VMEM)
SMEM = pl.BlockSpec(memory_space=pltpu.SMEM)
ANY = pl.BlockSpec(memory_space=pl.ANY)
F32 = jnp.float32
BF16 = jnp.bfloat16


def iota(shape, dim):
    return lax.broadcasted_iota(jnp.int32, shape, dim)


def params():
    return pltpu.CompilerParams(vmem_limit_bytes=56 * 1024 * 1024)


def rms_scale(inputs, gain_vec):
    mean_sq = jnp.mean(inputs * inputs, axis=-1, keepdims=True)
    return inputs * lax.rsqrt(mean_sq + EPS) * gain_vec


def attention_kernel(
    start_ref, sink_ref, q_ref, k_ref, v_ref, rim_ref, w_hbm, gain_ref, out_ref, w_vmem, mix, sem
):
    load = pltpu.make_async_copy(w_hbm, w_vmem, sem)
    load.start()
    group_size = HEADS // KV_HEADS
    blocks = q_ref.shape[0] // WINDOW
    kv_width = KV_HEADS * HEAD_DIM
    shape = (WINDOW, 2 * WINDOW)
    gap = iota(shape, 0) + WINDOW - iota(shape, 1)
    inside = (gap >= 0) & (gap < WINDOW)
    for n in range(blocks):
        rows = pl.ds(n * WINDOW, WINDOW)
        if n == 0:
            valid = inside & (iota(shape, 1) + start_ref[0] >= WINDOW)
        else:
            valid = inside
        for g in range(KV_HEADS):
            cols = pl.ds(g * HEAD_DIM, HEAD_DIM)
            if n == 0:
                keys = jnp.concatenate([rim_ref[:, cols], k_ref[rows, cols]], axis=0)
                rim_cols = pl.ds(kv_width + g * HEAD_DIM, HEAD_DIM)
                values = jnp.concatenate([rim_ref[:, rim_cols], v_ref[rows, cols]], axis=0)
            else:
                band = pl.ds((n - 1) * WINDOW, 2 * WINDOW)
                keys, values = k_ref[band, cols], v_ref[band, cols]
            mixed = []
            for j in range(group_size):
                h = g * group_size + j
                query = q_ref[rows, pl.ds(h * HEAD_DIM, HEAD_DIM)]
                scores = lax.dot_general(
                    query, keys, (((1,), (1,)), ((), ())), preferred_element_type=F32
                ) * (1.0 / math.sqrt(HEAD_DIM))
                scores = jnp.where(valid, scores, NEGATIVE)
                sink = sink_ref[h]
                top = jnp.maximum(jnp.max(scores, axis=-1, keepdims=True), sink)
                weights = jnp.exp(scores - top)
                total = jnp.sum(weights, axis=-1, keepdims=True) + jnp.exp(sink - top)
                probs = (weights * (1.0 / total)).astype(BF16)
                mixed.append(jnp.dot(probs, values, preferred_element_type=F32).astype(BF16))
            width = group_size * HEAD_DIM
            mix[rows, pl.ds(g * width, width)] = jnp.concatenate(mixed, axis=1)
    load.wait()
    for n in range(blocks):
        rows = pl.ds(n * WINDOW, WINDOW)
        projected = jnp.dot(mix[rows, :], w_vmem[...], preferred_element_type=F32)
        out_ref[rows, :] = rms_scale(projected, gain_ref[...]).astype(BF16)


def attention(att_queries, att_keys, att_values, rim, sink_logits, out_weight, att_gain, start):
    rows, width = att_queries.shape
    d = out_weight.shape[1]
    return pl.pallas_call(
        attention_kernel,
        out_shape=jax.ShapeDtypeStruct((rows, d), BF16),
        in_specs=[SMEM, SMEM, VMEM, VMEM, VMEM, VMEM, ANY, VMEM],
        out_specs=VMEM,
        scratch_shapes=[
            pltpu.VMEM(out_weight.shape, BF16),
            pltpu.VMEM((rows, width), BF16),
            pltpu.SemaphoreType.DMA,
        ],
        compiler_params=params(),
        cost_estimate=pl.CostEstimate(
            flops=12_000_000_000, bytes_accessed=8_000_000, transcendentals=2_000_000
        ),
        name="attention",
    )(start, sink_logits, att_queries, att_keys, att_values, rim, out_weight, att_gain[None])


def pack_block(slot_cap, plane, ids_ref, normed, packed_ref):
    tokens = normed.shape[0]
    slots = packed_ref.shape[0]
    groups = slots // slot_cap
    numbers = iota((groups, tokens), 0) * PLANES + plane
    hit = numbers == ids_ref[0:1, :]
    for k in range(1, ids_ref.shape[0]):
        hit = hit | (numbers == ids_ref[k : k + 1, :])
    earlier = (iota((tokens, tokens), 0) < iota((tokens, tokens), 1)).astype(F32).astype(BF16)
    before = jnp.dot(hit.astype(F32).astype(BF16), earlier, preferred_element_type=F32)
    place = jnp.where(hit, before + 1.0, 0.0).astype(BF16)
    from_slot = iota((slots, groups), 0) - iota((slots, groups), 1) * slot_cap
    spread = ((from_slot >= 0) & (from_slot < slot_cap)).astype(F32).astype(BF16)
    wanted = lax.rem(iota((slots, tokens), 0), slot_cap).astype(F32) + 1.0
    chosen = jnp.dot(spread, place, preferred_element_type=F32) == wanted
    chosen = chosen.astype(F32).astype(BF16)
    step = slots // 2
    for i in range(2):
        packed_ref[i * step : (i + 1) * step, :] = jnp.dot(
            chosen[i * step : (i + 1) * step], normed, preferred_element_type=F32
        ).astype(BF16)


def norm_pack_kernel(slot_cap, plane_ref, ids_ref, x_ref, gain_ref, normed_ref, packed_ref):
    normed = rms_scale(x_ref[...].astype(F32), gain_ref[...]).astype(BF16)
    normed_ref[...] = normed
    pack_block(slot_cap, plane_ref[0], ids_ref, normed, packed_ref)


def pack_kernel(slot_cap, plane_ref, ids_ref, normed_ref, packed_ref):
    pack_block(slot_cap, plane_ref[0], ids_ref, normed_ref[...], packed_ref)


def small_cost(flops=1_000_000_000):
    return pl.CostEstimate(flops=flops, bytes_accessed=2_000_000, transcendentals=0)


def norm_pack(moe_in, pre_gain, ids_t, plane, slot_cap, slots):
    tokens, d = moe_in.shape
    return pl.pallas_call(
        functools.partial(norm_pack_kernel, slot_cap),
        out_shape=(
            jax.ShapeDtypeStruct((tokens, d), BF16),
            jax.ShapeDtypeStruct((slots, d), BF16),
        ),
        in_specs=[SMEM] + [VMEM] * 3,
        out_specs=(VMEM, VMEM),
        compiler_params=params(),
        cost_estimate=small_cost(),
        name="norm_pack",
    )(plane, ids_t, moe_in, pre_gain[None])


def pack(normed, ids_t, plane, slot_cap, slots):
    return pl.pallas_call(
        functools.partial(pack_kernel, slot_cap),
        out_shape=jax.ShapeDtypeStruct((slots, normed.shape[1]), BF16),
        in_specs=[SMEM] + [VMEM] * 2,
        out_specs=VMEM,
        compiler_params=params(),
        cost_estimate=small_cost(),
        name="pack",
    )(plane, ids_t, normed)


def mlp_kernel(blocks, inputs, transposed, *refs):
    rows_refs, refs = refs[:inputs], refs[inputs:]
    gates, ups, downs = (refs[i * blocks : (i + 1) * blocks] for i in range(3))
    refs = refs[3 * blocks :]
    out_refs, refs = refs[:inputs], refs[inputs:]
    g_vmem, u_vmem, d_vmem, hidden, sems = refs
    width = d_vmem.shape[0] // blocks
    loads = []
    for b in range(blocks):
        loads.append(pltpu.make_async_copy(gates[b], g_vmem.at[b], sems.at[b]))
        loads.append(pltpu.make_async_copy(ups[b], u_vmem.at[b], sems.at[blocks + b]))
    for b in range(blocks):
        slot = d_vmem.at[pl.ds(b * width, width)]
        loads.append(pltpu.make_async_copy(downs[b], slot, sems.at[2 * blocks + b]))
    for load in loads:
        load.start()
    dims = (((1,), (1 if transposed else 0,)), ((), ()))
    total = rows_refs[0].shape[0]
    for b in range(blocks):
        loads[2 * b].wait()
        loads[2 * b + 1].wait()
        for i in range(inputs):
            rows = rows_refs[i][...]
            gate = lax.dot_general(rows, g_vmem[b], dims, preferred_element_type=F32)
            up = lax.dot_general(rows, u_vmem[b], dims, preferred_element_type=F32)
            hidden[b, i * total : (i + 1) * total, :] = (
                gate / (1.0 + jnp.exp(-gate)) * up
            ).astype(BF16)
    for load in loads[2 * blocks :]:
        load.wait()
    for i in range(inputs):
        units = jnp.concatenate(
            [hidden[b, i * total : (i + 1) * total, :] for b in range(blocks)], axis=1
        )
        out_refs[i][...] = jnp.dot(units, d_vmem[...], preferred_element_type=F32).astype(
            out_refs[i].dtype
        )


def mlp(rows, gates, ups, downs, transposed, dtype, name):
    total, d = rows[0].shape
    blocks, inputs = len(gates), len(rows)
    width = downs[0].shape[0]
    all_rows = total * inputs
    return pl.pallas_call(
        functools.partial(mlp_kernel, blocks, inputs, transposed),
        out_shape=[jax.ShapeDtypeStruct((total, d), dtype)] * inputs,
        in_specs=[VMEM] * inputs + [ANY] * (3 * blocks),
        out_specs=[VMEM] * inputs,
        scratch_shapes=[
            pltpu.VMEM((blocks,) + gates[0].shape, BF16),
            pltpu.VMEM((blocks,) + gates[0].shape, BF16),
            pltpu.VMEM((blocks * width, d), BF16),
            pltpu.VMEM((blocks, all_rows, width), BF16),
            pltpu.SemaphoreType.DMA((3 * blocks,)),
        ],
        compiler_params=params(),
        cost_estimate=pl.CostEstimate(
            flops=6 * all_rows * d * width * blocks,
            bytes_accessed=6 * d * width * blocks + 4 * all_rows * d,
            transcendentals=all_rows * width * blocks,
        ),
        name=name,
    )(*rows, *gates, *ups, *downs)


def partial_sum(slot_cap, plane, ids_ref, weight_ref, returned_ref, shared_ref):
    tokens, top_count = ids_ref.shape
    slots = returned_ref.shape[0]
    groups = slots // slot_cap
    index = iota((tokens, groups), 1)
    hits = [index * PLANES + plane == ids_ref[:, k : k + 1] for k in range(top_count)]
    hit = functools.reduce(lambda a, b: a | b, hits)
    earlier = (iota((tokens, tokens), 0) > iota((tokens, tokens), 1)).astype(F32).astype(BF16)
    before = jnp.dot(earlier, hit.astype(F32).astype(BF16), preferred_element_type=F32)
    place = before + (index * slot_cap + 1).astype(F32)
    lanes = iota((tokens, slots), 1).astype(F32) + 1.0
    combined = shared_ref[...]
    for k in range(top_count):
        slot = jnp.sum(jnp.where(hits[k], place, 0.0), axis=1, keepdims=True)
        chosen = (lanes == slot).astype(F32).astype(BF16)
        picked = jnp.dot(chosen, returned_ref[...], preferred_element_type=F32)
        combined = combined + weight_ref[:, k : k + 1] * picked
    return combined


def part_kernel(slot_cap, plane_ref, ids_ref, weight_ref, returned_ref, shared_ref, out_ref):
    out_ref[...] = partial_sum(
        slot_cap, plane_ref[0], ids_ref, weight_ref, returned_ref, shared_ref
    ).astype(BF16)


def final_kernel(
    slot_cap,
    plane_ref,
    ids_ref,
    weight_ref,
    returned_ref,
    shared_ref,
    other_ref,
    gain_ref,
    out_ref,
):
    combined = partial_sum(slot_cap, plane_ref[0], ids_ref, weight_ref, returned_ref, shared_ref)
    combined = combined + other_ref[...].astype(F32)
    out_ref[...] = rms_scale(combined, gain_ref[...]).astype(BF16)


def combine(kernel, name, slot_cap, plane, *arrays):
    return pl.pallas_call(
        functools.partial(kernel, slot_cap),
        out_shape=jax.ShapeDtypeStruct(arrays[3].shape, BF16),
        in_specs=[SMEM] + [VMEM] * len(arrays),
        out_specs=VMEM,
        compiler_params=params(),
        cost_estimate=small_cost(),
        name=name,
    )(plane, *arrays)


def swap(array, distance):
    size = lax.axis_size("tp")
    return lax.ppermute(array, "tp", [(i, i ^ distance) for i in range(size)])


def doubled(held, distance):
    while distance >= 1:
        held = held + [swap(block, distance) for block in held]
        distance //= 2
    return held


def one_expert(stacked, plane, far):
    kept = lax.dynamic_index_in_dim(stacked, plane, 0, keepdims=False)
    sent = lax.dynamic_index_in_dim(stacked, 1 - plane, 0, keepdims=False)
    return doubled([kept, swap(sent, far)], far // 2)


def exchange(array):
    return lax.all_to_all(array, "ep", split_axis=0, concat_axis=0, tiled=True)


def body(
    att_queries,
    att_keys,
    att_values,
    sink_logits,
    out_weight,
    att_gain,
    moe_in,
    pre_gain,
    expert_ids,
    routed_expert_weight,
    w_gate,
    w_up,
    w_down,
    common_expert_gate_weight,
    common_expert_up_weight,
    common_expert_down_weight,
    moe_gain,
):
    assert w_gate.shape[0] == PLANES
    devices = lax.axis_size(("ep", "tp"))
    tok_rows = att_queries.shape[0]
    tokens = moe_in.shape[0]
    top_count = expert_ids.shape[1]
    groups = lax.axis_size("ep")
    slot_cap = 2 * tokens * top_count // (PLANES * groups)
    slots = slot_cap * groups
    far = lax.axis_size("tp") // PLANES
    plane = (lax.axis_index("tp") // far).astype(jnp.int32)
    plane_arg = plane.reshape(1)

    edge = tok_rows - WINDOW
    rim = lax.ppermute(
        jnp.concatenate([att_keys[edge:], att_values[edge:]], axis=1),
        ("ep", "tp"),
        [(i, i + 1) for i in range(devices - 1)],
    )
    far_ids = swap(expert_ids, far)
    far_weight = swap(routed_expert_weight, far)

    far_ids_t = far_ids.T
    far_ids_t, far_ids, far_weight, rim, w_gate, moe_in = lax.optimization_barrier(
        (far_ids_t, far_ids, far_weight, rim, w_gate, moe_in)
    )

    normed, packed = norm_pack(moe_in, pre_gain, expert_ids.T, plane_arg, slot_cap, slots)
    far_normed = swap(normed, far)
    arrived = exchange(packed)
    far_packed = pack(far_normed, far_ids_t, plane_arg, slot_cap, slots)
    start = (lax.axis_index(("ep", "tp")) * tok_rows).astype(jnp.int32).reshape(1)
    mixer_out = attention(
        att_queries, att_keys, att_values, rim, sink_logits, out_weight, att_gain, start
    )
    far_packed, mixer_out = lax.optimization_barrier((far_packed, mixer_out))
    far_arrived = exchange(far_packed)

    gates = one_expert(jnp.swapaxes(w_gate, 1, 2), plane, far)
    w_up, w_down, far_normed = lax.optimization_barrier((w_up, w_down, far_normed))
    ups = one_expert(jnp.swapaxes(w_up, 1, 2), plane, far)
    downs = one_expert(w_down, plane, far)
    common_gates = doubled([common_expert_gate_weight], far // 2)
    common_ups = doubled([common_expert_up_weight], far // 2)
    common_downs = doubled([common_expert_down_weight], far // 2)

    shared_own, shared_far = mlp(
        [normed, far_normed], common_gates, common_ups, common_downs, False, F32, "shared"
    )
    far_arrived, arrived, shared_own, shared_far = lax.optimization_barrier(
        (far_arrived, arrived, shared_own, shared_far)
    )

    (far_outputs,) = mlp([far_arrived], gates, ups, downs, True, BF16, "far_expert")
    far_returned = exchange(far_outputs)
    (outputs,) = mlp([arrived], gates, ups, downs, True, BF16, "own_expert")
    returned = exchange(outputs)
    far_part = combine(
        part_kernel, "far_part", slot_cap, plane_arg, far_ids, far_weight, far_returned, shared_far
    )
    other = swap(far_part, far)
    experts_out = combine(
        final_kernel,
        "final",
        slot_cap,
        plane_arg,
        expert_ids,
        routed_expert_weight,
        returned,
        shared_own,
        other,
        moe_gain[None],
    )
    return (mixer_out, experts_out)


def solution(mesh):
    in_specs = (
        P(("ep", "tp"), None),
        P(("ep", "tp"), None),
        P(("ep", "tp"), None),
        P(),
        P(),
        P(),
        P(("ep", "tp"), None),
        P(),
        P(("ep", "tp"), None),
        P(("ep", "tp"), None),
        P("ep", None, "tp"),
        P("ep", None, "tp"),
        P("ep", "tp", None),
        P(None, "tp"),
        P(None, "tp"),
        P("tp", None),
        P(),
    )
    out_specs = (P(("ep", "tp"), None), P(("ep", "tp"), None))
    return jax.shard_map(body, mesh=mesh, in_specs=in_specs, out_specs=out_specs, check_vma=False)
```
